32 devices in a mesh: sp: 8 (over z, y), tp: 4 (over x, core).
Axes of the slice: x: 2, y: 2, z: 4, core: 2. Of those that a mesh axis runs over, the one named last changes fastest.
Arguments:
- tokens: bfloat16 [4096, 2048], P(('sp', 'tp')), may hold values from -6 to 6
- norm_gain: float32 [2048], replicated, may hold values from 0.1 to 1.9
- query_weight: bfloat16 [2048, 2048], P('sp', 'tp'), may hold values from -0.125 to 0.125
- key_weight: bfloat16 [2048, 2048], P('sp', 'tp'), may hold values from -0.125 to 0.125
- value_weight: bfloat16 [2048, 4096], P('sp', 'tp'), may hold values from -0.125 to 0.125
- retain_gate: bfloat16 [2048, 4096], P('sp', 'tp'), may hold values from -0.125 to 0.125
- unit_value: bfloat16 [2048, 2048], P('sp', 'tp'), may hold values from -0.125 to 0.125
- unit_gate: bfloat16 [2048, 2048], P('sp', 'tp'), may hold values from -0.125 to 0.125
- convolve_gate: bfloat16 [2048, 2048], P('sp', 'tp'), may hold values from -0.125 to 0.125
- filter_taps: float32 [31, 2048], replicated, may hold values from -1 to 1
- layer_gain: float32 [2048], replicated, may hold values from 0.1 to 1.9
- layer_shift: float32 [2048], replicated, may hold values from -3 to 3
- retain_output: bfloat16 [2048, 4096], P('sp', 'tp'), may hold values from -0.09375 to 0.09375
- convolve_output: bfloat16 [2048, 2048], P('sp', 'tp'), may hold values from -0.125 to 0.125
Outputs:
- mixed: bfloat16 [4096, 2048], P(('sp', 'tp'))
The draws below stay inside these ranges and needn't reach their ends.
All inputs are finite; a program needn't handle non-finite values.
Results may differ from the reference program's by a relative error of at most 0.018.
Values may be sent and summed in bfloat16 or wider, within the bound.
A program may use at most 128 MiB of HBM per device.

```python
import jax
import jax.numpy as jnp
from jax import lax

D = 2048
HEADS = 8
KEY = 256
VAL = 512
CONV = 2048
GROUP = 512
KW = 31
TOK_DEV = 512
QK = 2048
VW = 4096
SEQ = 4096


def steps_of(stream_key, shape, cuts, smallest, top_value):
    gain, own = 1.0, jax.random.fold_in(stream_key, 6)
    for dim, shards_of in cuts:
        draws = jnp.exp(jax.random.uniform(jax.random.fold_in(own, dim), (shards_of,), jnp.float32, smallest / len(cuts), top_value / len(cuts)))
        gain = gain * jnp.repeat(draws, shape[dim] // shards_of).reshape([-1 if axis == dim else 1 for axis in range(len(shape))])
    return gain


def centred(own_key, extent, scale, most, shards=(), kind=jnp.bfloat16):
    drawn = jax.random.normal(own_key, extent, jnp.float32) * scale
    if len(shards) > 0:
        drawn = steps_of(own_key, extent, shards, -0.22, 0.18) * drawn
    return jnp.clip(drawn, min=-most, max=most).astype(kind)


def setup_inputs(seed: int = 0) -> dict:
    keys = jax.random.split(jax.random.key(seed), 15)
    return {
        "tokens": centred(keys[0], (SEQ, D), 1.0, 6.0, ((0, 32),)),
        "norm_gain": jnp.clip(1.0 + 0.18 * jax.random.normal(keys[1], (D,), jnp.float32), 0.1, 1.9),
        "query_weight": centred(keys[2], (D, QK), D ** -0.5, 0.125, ((0, 8), (1, 4))),
        "key_weight": centred(keys[3], (D, QK), D ** -0.5, 0.125, ((0, 8), (1, 4))),
        "value_weight": centred(keys[4], (D, VW), D ** -0.5, 0.125, ((0, 8), (1, 4))),
        "retain_gate": centred(keys[5], (D, VW), D ** -0.5, 0.125, ((0, 8), (1, 4))),
        "unit_value": centred(keys[6], (D, CONV), D ** -0.5, 0.125, ((0, 8), (1, 4))),
        "unit_gate": centred(keys[7], (D, CONV), D ** -0.5, 0.125, ((0, 8), (1, 4))),
        "convolve_gate": centred(keys[8], (D, CONV), D ** -0.5, 0.125, ((0, 8), (1, 4))),
        "filter_taps": centred(keys[9], (KW, CONV), KW ** -0.5, 1.0, (), jnp.float32),
        "layer_gain": jnp.clip(1.0 + 0.18 * jax.random.normal(keys[10], (CONV,), jnp.float32), 0.1, 1.9),
        "layer_shift": centred(keys[11], (CONV,), 0.5, 3.0, (), jnp.float32),
        "retain_output": centred(keys[12], (D, VW), VW ** -0.5, 0.09375, ((0, 8), (1, 4))),
        "convolve_output": centred(keys[13], (D, CONV), CONV ** -0.5, 0.125, ((0, 8), (1, 4))),
    }


rms_eps = 1e-06
group_eps = 1.0
layer_eps = 0.001
rope_base = 10000.0
highest = lax.Precision.HIGHEST

def rms_normalize(tokens, norm_gain):
    widened = tokens.astype(jnp.float32)
    scaled = widened * lax.rsqrt(lax.optimization_barrier(jnp.mean(widened * widened, axis=-1, keepdims=True)) + rms_eps)
    return (scaled * norm_gain).astype(jnp.bfloat16)

def widen(narrow_value):
    return lax.optimization_barrier(narrow_value.astype(jnp.bfloat16)).astype(jnp.float32)

def rotate(vectors, positions):
    half_width = vectors.shape[-1] // 2
    frequency = rope_base ** (-jnp.arange(half_width, dtype=jnp.float32) / half_width)
    angles = positions.astype(jnp.float32)[:, None] * frequency
    cosine = jnp.cos(angles)[:, None, :]
    sine_part = jnp.sin(angles)[:, None, :]
    front_half = vectors[..., :half_width]
    back_half = vectors[..., half_width:]
    return jnp.concatenate([front_half * cosine - back_half * sine_part, front_half * sine_part + back_half * cosine], axis=-1)

def prepare(queries, key_rows, values, positions):
    row_count = queries.shape[0]
    rotated_query = widen(rotate(queries.astype(jnp.float32).reshape(row_count, -1, KEY), positions))
    rotated_keys = widen(rotate(key_rows.astype(jnp.float32).reshape(row_count, -1, KEY), positions) * KEY ** (-0.5))
    value_heads = values.astype(jnp.float32).reshape(row_count, -1, VAL)
    return (rotated_query, rotated_keys, value_heads)

def decay_logs(first_head, head_total, all_heads, seq_length):
    ratio = (first_head + jnp.arange(head_total)).astype(jnp.float32) / (all_heads - 1)
    return (jnp.log(0.05) + ratio * jnp.log(18.0)) / seq_length

def local_parts(queries, key_rows, values, log_decay):
    row_count = queries.shape[0]
    indices = jnp.arange(row_count, dtype=jnp.float32)
    offsets = indices[:, None] - indices[None, :]
    causal = offsets >= 0
    weight = jnp.where(causal[None], jnp.exp(log_decay[:, None, None] * jnp.where(causal, offsets, 0.0)[None]), 0.0)
    scores = widen(jnp.einsum('ihd,jhd->hij', queries, key_rows) * weight)
    within = jnp.einsum('hij,jhe->ihe', scores, values)
    trailing = jnp.exp(log_decay[None, :] * (row_count - 1.0 - indices)[:, None])
    weighted = widen(key_rows * trailing[:, :, None])
    contribution = jnp.einsum('jhd,jhe->hde', weighted, values)
    return (within, contribution)

def cross_part(queries, carry_state, log_decay):
    row_count = queries.shape[0]
    indices = jnp.arange(row_count, dtype=jnp.float32)
    leading = jnp.exp(log_decay[None, :] * (indices + 1.0)[:, None])
    return jnp.einsum('ihd,hde->ihe', queries, carry_state, precision=highest) * leading[:, :, None]

def retain_finish(raw, switch):
    average = lax.optimization_barrier(jnp.mean(raw, axis=-1, keepdims=True))
    spread = lax.optimization_barrier(jnp.mean(jnp.square(raw - average), axis=-1, keepdims=True))
    normalized = ((raw - average) * lax.rsqrt(spread + group_eps)).reshape(raw.shape[0], -1)
    return (normalized * jax.nn.silu(switch.astype(jnp.float32))).astype(jnp.bfloat16)

def convolve_branch(gated_input, before, tap_slice, gain_slice, shift_slice, switch):
    padded = jnp.concatenate([before, gated_input], axis=0)
    row_count = gated_input.shape[0]
    summed = jnp.zeros(gated_input.shape, jnp.float32)
    for tap_index in range(tap_slice.shape[0]):
        summed = summed + padded[tap_index:tap_index + row_count].astype(jnp.float32) * tap_slice[tap_index]
    grouped = summed.reshape(row_count, -1, GROUP)
    average = lax.optimization_barrier(jnp.mean(grouped, axis=-1, keepdims=True))
    spread = lax.optimization_barrier(jnp.mean(jnp.square(grouped - average), axis=-1, keepdims=True))
    normalized = ((grouped - average) * lax.rsqrt(spread + layer_eps)).reshape(row_count, -1)
    normalized = normalized * gain_slice + shift_slice
    return (jax.nn.silu(normalized) * jax.nn.silu(switch.astype(jnp.float32))).astype(jnp.bfloat16)

def contract(hidden, matrix):
    return lax.dot_general(hidden, matrix, (((1,), (1,)), ((), ())), preferred_element_type=jnp.float32)

def reference(tokens, norm_gain, query_weight, key_weight, value_weight, retain_gate, unit_value, unit_gate, convolve_gate, filter_taps, layer_gain, layer_shift, retain_output, convolve_output):
    seq_total = tokens.shape[0]
    normed = rms_normalize(tokens, norm_gain)

    def project(matrix):
        return jnp.dot(normed, matrix, preferred_element_type=jnp.float32).astype(jnp.bfloat16)
    queries = project(query_weight)
    key_rows = project(key_weight)
    values = project(value_weight)
    retain_switch = project(retain_gate)
    glu_value = project(unit_value)
    glu_switch = project(unit_gate)
    convolve_switch = project(convolve_gate)
    positions = jnp.arange(seq_total, dtype=jnp.int32)
    rotated_query, rotated_keys, value_heads = prepare(queries, key_rows, values, positions)
    log_decay = decay_logs(0, HEADS, HEADS, seq_total)
    totals = jnp.exp(log_decay * TOK_DEV)
    blocks = seq_total // TOK_DEV

    def advance(carry_state, block):
        block_query, block_keys, block_values = block
        within, contribution = local_parts(block_query, block_keys, block_values, log_decay)
        result = within + cross_part(block_query, carry_state, log_decay)
        return (carry_state * totals[:, None, None] + contribution, result)
    start_state = jnp.zeros((HEADS, KEY, VAL), jnp.float32)
    final_state, outputs = lax.scan(advance, start_state, (rotated_query.reshape(blocks, TOK_DEV, HEADS, KEY), rotated_keys.reshape(blocks, TOK_DEV, HEADS, KEY), value_heads.reshape(blocks, TOK_DEV, HEADS, VAL)))
    raw = outputs.reshape(seq_total, HEADS, VAL)
    retain_hidden = retain_finish(raw, retain_switch)
    gated_input = (glu_value.astype(jnp.float32) * jax.nn.sigmoid(glu_switch.astype(jnp.float32))).astype(jnp.bfloat16)
    before = jnp.zeros((KW - 1, CONV), jnp.bfloat16)
    convolve_hidden = convolve_branch(gated_input, before, filter_taps, layer_gain, layer_shift, convolve_switch)
    summed = contract(retain_hidden, retain_output) + contract(convolve_hidden, convolve_output)
    return summed.astype(jnp.bfloat16)
```

```python
import jax
import jax.numpy as jnp
from jax import lax
from jax.sharding import Mesh
from jax.sharding import PartitionSpec as P

KEY = 256
VAL = 512
GROUP = 512
KW = 31


rms_eps = 1e-06
group_eps = 1.0
layer_eps = 0.001
rope_base = 10000.0


SPANS = ("tp", "lo")


def swap_planes(x):
    size = lax.axis_size("tp")
    pairs = [(h * size + t, t * size + h) for h in range(size) for t in range(size)]
    return lax.ppermute(x, ("hi", "tp"), pairs)


def swap_planes_rolled(x):
    size = lax.axis_size("tp")
    pairs = [
        (h * size + t, t * size + (h + size // 2) % size)
        for h in range(size)
        for t in range(size)
    ]
    return lax.ppermute(x, ("hi", "tp"), pairs)


def from_behind(x, by):
    outer, inner = lax.axis_size("tp"), lax.axis_size("lo")
    spot = [(i % inner) * outer + i // inner for i in range(outer * inner)]
    return lax.ppermute(x, ("lo", "tp"), list(zip(spot[:-by], spot[by:])))


def carried_in(contribution, log_span_decay):
    length = lax.axis_size(SPANS)
    state = from_behind(contribution.astype(jnp.bfloat16), 1).astype(jnp.float32)
    by = 1
    while by < length:
        earlier = from_behind(state.astype(jnp.bfloat16), by).astype(jnp.float32)
        state = state + jnp.exp(log_span_decay * by)[:, None, None] * earlier
        by *= 2
    return state


def rms_normalize(tokens, norm_gain):
    widened = tokens.astype(jnp.float32)
    scaled = widened * lax.rsqrt(jnp.mean(widened * widened, axis=-1, keepdims=True) + rms_eps)
    return (scaled * norm_gain).astype(jnp.bfloat16)


def rotate(vectors, positions):
    half_width = vectors.shape[-1] // 2
    frequency = rope_base ** (-jnp.arange(half_width, dtype=jnp.float32) / half_width)
    angles = positions.astype(jnp.float32)[:, None] * frequency
    cosine = jnp.cos(angles)[:, None, :]
    sine_part = jnp.sin(angles)[:, None, :]
    front_half = vectors[..., :half_width]
    back_half = vectors[..., half_width:]
    return jnp.concatenate(
        [front_half * cosine - back_half * sine_part, front_half * sine_part + back_half * cosine],
        axis=-1,
    )


def prepare(queries, key_rows, values, positions):
    row_count = queries.shape[0]
    rotated_query = rotate(
        queries.astype(jnp.float32).reshape(row_count, -1, KEY), positions
    ).astype(jnp.bfloat16)
    rotated_keys = (
        rotate(key_rows.astype(jnp.float32).reshape(row_count, -1, KEY), positions) * KEY ** (-0.5)
    ).astype(jnp.bfloat16)
    value_heads = values.reshape(row_count, -1, VAL)
    return (rotated_query, rotated_keys, value_heads)


def decay_logs(first_head, head_total, all_heads, seq_length):
    ratio = (first_head + jnp.arange(head_total)).astype(jnp.float32) / (all_heads - 1)
    return (jnp.log(0.05) + ratio * jnp.log(18.0)) / seq_length


def local_parts(queries, key_rows, values, log_decay):
    row_count = queries.shape[0]
    indices = jnp.arange(row_count, dtype=jnp.float32)
    offsets = indices[:, None] - indices[None, :]
    causal = offsets >= 0
    weight = jnp.where(
        causal[None], jnp.exp(log_decay[:, None, None] * jnp.where(causal, offsets, 0.0)[None]), 0.0
    )
    scores = (
        jnp.einsum("ihd,jhd->hij", queries, key_rows, preferred_element_type=jnp.float32) * weight
    ).astype(jnp.bfloat16)
    within = jnp.einsum("hij,jhe->ihe", scores, values, preferred_element_type=jnp.float32)
    trailing = jnp.exp(log_decay[None, :] * (row_count - 1.0 - indices)[:, None])
    weighted = (key_rows.astype(jnp.float32) * trailing[:, :, None]).astype(jnp.bfloat16)
    contribution = jnp.einsum("jhd,jhe->hde", weighted, values, preferred_element_type=jnp.float32)
    return (within, contribution)


def cross_part(queries, carry_state, log_decay):
    row_count = queries.shape[0]
    indices = jnp.arange(row_count, dtype=jnp.float32)
    leading = jnp.exp(log_decay[None, :] * (indices + 1.0)[:, None])
    return (
        jnp.einsum(
            "ihd,hde->ihe",
            queries,
            carry_state.astype(jnp.bfloat16),
            preferred_element_type=jnp.float32,
        )
        * leading[:, :, None]
    )


def retain_finish(raw, switch):
    average = jnp.mean(raw, axis=-1, keepdims=True)
    spread = jnp.mean(jnp.square(raw - average), axis=-1, keepdims=True)
    normalized = ((raw - average) * lax.rsqrt(spread + group_eps)).reshape(raw.shape[0], -1)
    return (normalized * jax.nn.silu(switch.astype(jnp.float32))).astype(jnp.bfloat16)


def convolve_branch(gated_input, before, tap_slice, gain_slice, shift_slice, switch):
    padded = jnp.concatenate([before, gated_input], axis=0)
    row_count = gated_input.shape[0]
    summed = jnp.zeros(gated_input.shape, jnp.float32)
    for tap_index in range(tap_slice.shape[0]):
        summed = (
            summed
            + padded[tap_index : tap_index + row_count].astype(jnp.float32) * tap_slice[tap_index]
        )
    grouped = summed.reshape(row_count, -1, GROUP)
    average = jnp.mean(grouped, axis=-1, keepdims=True)
    spread = jnp.mean(jnp.square(grouped - average), axis=-1, keepdims=True)
    normalized = ((grouped - average) * lax.rsqrt(spread + layer_eps)).reshape(row_count, -1)
    normalized = normalized * gain_slice + shift_slice
    return (jax.nn.silu(normalized) * jax.nn.silu(switch.astype(jnp.float32))).astype(jnp.bfloat16)


def contract(hidden, matrix):
    return lax.dot_general(
        hidden, matrix, (((1,), (1,)), ((), ())), preferred_element_type=jnp.float32
    )


def local(
    tokens,
    norm_gain,
    query_weight,
    key_weight,
    value_weight,
    retain_gate,
    unit_value,
    unit_gate,
    convolve_gate,
    filter_taps,
    layer_gain,
    layer_shift,
    retain_output,
    convolve_output,
):
    head_groups = lax.axis_size("hi")
    chain_length = lax.axis_size(SPANS)
    head_rank = lax.axis_index("hi")
    chain_rank = lax.axis_index(SPANS)
    normed = lax.all_gather(
        swap_planes(rms_normalize(tokens, norm_gain)), "hi", axis=0, tiled=True
    )
    half = normed.shape[1] // 2
    normed_rolled = jnp.concatenate([normed[:, half:], normed[:, :half]], axis=1)

    def straight(matrix):
        return lax.all_gather(swap_planes(matrix), SPANS, axis=0, tiled=True)

    def rolled(matrix):
        return lax.all_gather(swap_planes_rolled(matrix), SPANS, axis=0, tiled=True)

    def project(rows, matrix):
        return jnp.dot(rows, matrix, preferred_element_type=jnp.float32).astype(jnp.bfloat16)

    key_rows = project(normed, straight(key_weight))
    values = project(normed_rolled, rolled(value_weight))
    queries = project(normed, straight(query_weight))
    glu_value = project(normed, straight(unit_value))
    glu_switch = project(normed_rolled, rolled(unit_gate))
    convolve_switch = project(normed, straight(convolve_gate))
    retain_switch = project(normed_rolled, rolled(retain_gate))
    convolve_full = rolled(convolve_output)
    retain_full = straight(retain_output)
    row_count = normed.shape[0]
    local_heads = queries.shape[1] // KEY
    positions = chain_rank * row_count + jnp.arange(row_count, dtype=jnp.int32)
    rotated_query, rotated_keys, value_heads = prepare(queries, key_rows, values, positions)
    log_decay = decay_logs(
        head_rank * local_heads, local_heads, local_heads * head_groups, row_count * chain_length
    )
    within, contribution = local_parts(rotated_query, rotated_keys, value_heads, log_decay)
    gated_input = (
        glu_value.astype(jnp.float32) * jax.nn.sigmoid(glu_switch.astype(jnp.float32))
    ).astype(jnp.bfloat16)
    channels = gated_input.shape[1]
    before = from_behind(gated_input[row_count - (KW - 1) :], 1)
    incoming = carried_in(contribution, log_decay * row_count)
    raw = within + cross_part(rotated_query, incoming, log_decay)
    retain_hidden = retain_finish(raw, retain_switch)
    tap_slice = lax.dynamic_slice_in_dim(filter_taps, head_rank * channels, channels, 1)
    gain_slice = lax.dynamic_slice_in_dim(layer_gain, head_rank * channels, channels, 0)
    shift_slice = lax.dynamic_slice_in_dim(layer_shift, head_rank * channels, channels, 0)
    convolve_hidden = convolve_branch(
        gated_input, before, tap_slice, gain_slice, shift_slice, convolve_switch
    )
    convolved_out = contract(convolve_hidden, convolve_full)
    convolved_out = jnp.concatenate([convolved_out[:, half:], convolved_out[:, :half]], axis=1)
    mixed = (contract(retain_hidden, retain_full) + convolved_out).astype(jnp.bfloat16)
    return swap_planes(lax.psum_scatter(mixed, "hi", scatter_dimension=0, tiled=True))


def solution(mesh):
    sp, tp = mesh.shape["sp"], mesh.shape["tp"]
    planes = Mesh(mesh.devices.reshape(tp, sp // tp, tp), ("hi", "lo", "tp"))
    return jax.shard_map(
        local,
        mesh=planes,
        in_specs=(
            P(("hi", "lo", "tp"), None),
            P(),
            P(("hi", "lo"), "tp"),
            P(("hi", "lo"), "tp"),
            P(("hi", "lo"), "tp"),
            P(("hi", "lo"), "tp"),
            P(("hi", "lo"), "tp"),
            P(("hi", "lo"), "tp"),
            P(("hi", "lo"), "tp"),
            P(),
            P(),
            P(),
            P(("hi", "lo"), "tp"),
            P(("hi", "lo"), "tp"),
        ),
        out_specs=P(("hi", "lo", "tp"), None),
        check_vma=False,
    )
```

```python
import jax
import jax.numpy as jnp
from jax import lax
from jax.sharding import Mesh
from jax.sharding import PartitionSpec as P

KEY = 256
VAL = 512
GROUP = 512
KW = 31


rms_eps = 1e-06
group_eps = 1.0
layer_eps = 0.001
rope_base = 10000.0


SPANS = ("tp", "lo")


def swap_planes(x):
    size = lax.axis_size("tp")
    pairs = [(h * size + t, t * size + h) for h in range(size) for t in range(size)]
    return lax.ppermute(x, ("hi", "tp"), pairs)


def swap_planes_rolled(x):
    size = lax.axis_size("tp")
    pairs = [
        (h * size + t, t * size + (h + size // 2) % size)
        for h in range(size)
        for t in range(size)
    ]
    return lax.ppermute(x, ("hi", "tp"), pairs)


def from_behind(x, by):
    outer, inner = lax.axis_size("tp"), lax.axis_size("lo")
    spot = [(i % inner) * outer + i // inner for i in range(outer * inner)]
    return lax.ppermute(x, ("lo", "tp"), list(zip(spot[:-by], spot[by:])))


def carried_in(contribution, log_span_decay):
    length = lax.axis_size(SPANS)
    state = from_behind(contribution.astype(jnp.bfloat16), 1).astype(jnp.float32)
    by = 1
    while by < length:
        earlier = from_behind(state.astype(jnp.bfloat16), by).astype(jnp.float32)
        state = state + jnp.exp(log_span_decay * by)[:, None, None] * earlier
        by *= 2
    return state


def rms_normalize(tokens, norm_gain):
    widened = tokens.astype(jnp.float32)
    scaled = widened * lax.rsqrt(jnp.mean(widened * widened, axis=-1, keepdims=True) + rms_eps)
    return (scaled * norm_gain).astype(jnp.bfloat16)


def rotate(vectors, positions):
    half_width = vectors.shape[-1] // 2
    frequency = rope_base ** (-jnp.arange(half_width, dtype=jnp.float32) / half_width)
    angles = positions.astype(jnp.float32)[:, None] * frequency
    cosine = jnp.cos(angles)[:, None, :]
    sine_part = jnp.sin(angles)[:, None, :]
    front_half = vectors[..., :half_width]
    back_half = vectors[..., half_width:]
    return jnp.concatenate(
        [front_half * cosine - back_half * sine_part, front_half * sine_part + back_half * cosine],
        axis=-1,
    )


def prepare(queries, key_rows, values, positions):
    row_count = queries.shape[0]
    rotated_query = rotate(
        queries.astype(jnp.float32).reshape(row_count, -1, KEY), positions
    ).astype(jnp.bfloat16)
    rotated_keys = (
        rotate(key_rows.astype(jnp.float32).reshape(row_count, -1, KEY), positions) * KEY ** (-0.5)
    ).astype(jnp.bfloat16)
    value_heads = values.reshape(row_count, -1, VAL)
    return (rotated_query, rotated_keys, value_heads)


def decay_logs(first_head, head_total, all_heads, seq_length):
    ratio = (first_head + jnp.arange(head_total)).astype(jnp.float32) / (all_heads - 1)
    return (jnp.log(0.05) + ratio * jnp.log(18.0)) / seq_length


def local_parts(queries, key_rows, values, log_decay):
    row_count = queries.shape[0]
    indices = jnp.arange(row_count, dtype=jnp.float32)
    offsets = indices[:, None] - indices[None, :]
    causal = offsets >= 0
    weight = jnp.where(
        causal[None], jnp.exp(log_decay[:, None, None] * jnp.where(causal, offsets, 0.0)[None]), 0.0
    )
    scores = (
        jnp.einsum("ihd,jhd->hij", queries, key_rows, preferred_element_type=jnp.float32) * weight
    ).astype(jnp.bfloat16)
    within = jnp.einsum("hij,jhe->ihe", scores, values, preferred_element_type=jnp.float32)
    trailing = jnp.exp(log_decay[None, :] * (row_count - 1.0 - indices)[:, None])
    weighted = (key_rows.astype(jnp.float32) * trailing[:, :, None]).astype(jnp.bfloat16)
    contribution = jnp.einsum("jhd,jhe->hde", weighted, values, preferred_element_type=jnp.float32)
    return (within, contribution)


def cross_part(queries, carry_state, log_decay):
    row_count = queries.shape[0]
    indices = jnp.arange(row_count, dtype=jnp.float32)
    leading = jnp.exp(log_decay[None, :] * (indices + 1.0)[:, None])
    return (
        jnp.einsum(
            "ihd,hde->ihe",
            queries,
            carry_state.astype(jnp.bfloat16),
            preferred_element_type=jnp.float32,
        )
        * leading[:, :, None]
    )


def retain_finish(raw, switch):
    average = jnp.mean(raw, axis=-1, keepdims=True)
    spread = jnp.mean(jnp.square(raw - average), axis=-1, keepdims=True)
    normalized = ((raw - average) * lax.rsqrt(spread + group_eps)).reshape(raw.shape[0], -1)
    return (normalized * jax.nn.silu(switch.astype(jnp.float32))).astype(jnp.bfloat16)


def convolve_branch(gated_input, before, tap_slice, gain_slice, shift_slice, switch):
    padded = jnp.concatenate([before, gated_input], axis=0)
    row_count = gated_input.shape[0]
    summed = jnp.zeros(gated_input.shape, jnp.float32)
    for tap_index in range(tap_slice.shape[0]):
        summed = (
            summed
            + padded[tap_index : tap_index + row_count].astype(jnp.float32) * tap_slice[tap_index]
        )
    grouped = summed.reshape(row_count, -1, GROUP)
    average = jnp.mean(grouped, axis=-1, keepdims=True)
    spread = jnp.mean(jnp.square(grouped - average), axis=-1, keepdims=True)
    normalized = ((grouped - average) * lax.rsqrt(spread + layer_eps)).reshape(row_count, -1)
    normalized = normalized * gain_slice + shift_slice
    return (jax.nn.silu(normalized) * jax.nn.silu(switch.astype(jnp.float32))).astype(jnp.bfloat16)


def contract(hidden, matrix):
    return lax.dot_general(
        hidden, matrix, (((1,), (1,)), ((), ())), preferred_element_type=jnp.float32
    )


def local(
    tokens,
    norm_gain,
    query_weight,
    key_weight,
    value_weight,
    retain_gate,
    unit_value,
    unit_gate,
    convolve_gate,
    filter_taps,
    layer_gain,
    layer_shift,
    retain_output,
    convolve_output,
):
    head_groups = lax.axis_size("hi")
    chain_length = lax.axis_size(SPANS)
    head_rank = lax.axis_index("hi")
    chain_rank = lax.axis_index(SPANS)
    normed = lax.all_gather(
        swap_planes(rms_normalize(tokens, norm_gain)), "hi", axis=0, tiled=True
    )
    half = normed.shape[1] // 2
    normed_rolled = jnp.concatenate([normed[:, half:], normed[:, :half]], axis=1)

    def gathered(swap, *matrices):
        return lax.all_gather(
            swap(jnp.concatenate(matrices, axis=1)), SPANS, axis=0, tiled=True
        )

    def project(rows, merged, *matrices):
        product = jnp.dot(rows, merged, preferred_element_type=jnp.float32).astype(jnp.bfloat16)
        ends = [sum(m.shape[1] for m in matrices[: k + 1]) for k in range(len(matrices) - 1)]
        return jnp.split(product, ends, axis=1)

    first = (key_weight, value_weight, query_weight)
    second = (unit_value, unit_gate, convolve_gate, retain_gate)
    third = (retain_output, convolve_output)
    key_rows, values, queries = project(normed, gathered(swap_planes, *first), *first)
    glu_value, glu_switch, convolve_switch, retain_switch = project(
        normed_rolled, gathered(swap_planes_rolled, *second), *second
    )
    out_full = gathered(swap_planes, *third)
    row_count = normed.shape[0]
    local_heads = queries.shape[1] // KEY
    positions = chain_rank * row_count + jnp.arange(row_count, dtype=jnp.int32)
    rotated_query, rotated_keys, value_heads = prepare(queries, key_rows, values, positions)
    log_decay = decay_logs(
        head_rank * local_heads, local_heads, local_heads * head_groups, row_count * chain_length
    )
    within, contribution = local_parts(rotated_query, rotated_keys, value_heads, log_decay)
    gated_input = (
        glu_value.astype(jnp.float32) * jax.nn.sigmoid(glu_switch.astype(jnp.float32))
    ).astype(jnp.bfloat16)
    channels = gated_input.shape[1]
    before = from_behind(gated_input[row_count - (KW - 1) :], 1)
    incoming = carried_in(contribution, log_decay * row_count)
    raw = within + cross_part(rotated_query, incoming, log_decay)
    retain_hidden = retain_finish(raw, retain_switch)
    tap_slice = lax.dynamic_slice_in_dim(filter_taps, head_rank * channels, channels, 1)
    gain_slice = lax.dynamic_slice_in_dim(layer_gain, head_rank * channels, channels, 0)
    shift_slice = lax.dynamic_slice_in_dim(layer_shift, head_rank * channels, channels, 0)
    convolve_hidden = convolve_branch(
        gated_input, before, tap_slice, gain_slice, shift_slice, convolve_switch
    )
    hidden = jnp.concatenate([retain_hidden, convolve_hidden], axis=1)
    mixed = contract(hidden, out_full).astype(jnp.bfloat16)
    return swap_planes(lax.psum_scatter(mixed, "hi", scatter_dimension=0, tiled=True))


def solution(mesh):
    sp, tp = mesh.shape["sp"], mesh.shape["tp"]
    planes = Mesh(mesh.devices.reshape(tp, sp // tp, tp), ("hi", "lo", "tp"))
    return jax.shard_map(
        local,
        mesh=planes,
        in_specs=(
            P(("hi", "lo", "tp"), None),
            P(),
            P(("hi", "lo"), "tp"),
            P(("hi", "lo"), "tp"),
            P(("hi", "lo"), "tp"),
            P(("hi", "lo"), "tp"),
            P(("hi", "lo"), "tp"),
            P(("hi", "lo"), "tp"),
            P(("hi", "lo"), "tp"),
            P(),
            P(),
            P(),
            P(("hi", "lo"), "tp"),
            P(("hi", "lo"), "tp"),
        ),
        out_specs=P(("hi", "lo", "tp"), None),
        check_vma=False,
    )
```

```python
import jax
import jax.numpy as jnp
from jax import lax
from jax.experimental import pallas as pl
from jax.experimental.pallas import tpu as pltpu
from jax.sharding import Mesh
from jax.sharding import PartitionSpec as P

KEY = 256
VAL = 512
GROUP = 512
KW = 31


rms_eps = 1e-06
group_eps = 1.0
layer_eps = 0.001
rope_base = 10000.0


SPANS = ("tp", "lo")


def swap_planes(x):
    size = lax.axis_size("tp")
    pairs = [(h * size + t, t * size + h) for h in range(size) for t in range(size)]
    return lax.ppermute(x, ("hi", "tp"), pairs)


def from_behind(x, by):
    outer, inner = lax.axis_size("tp"), lax.axis_size("lo")
    spot = [(i % inner) * outer + i // inner for i in range(outer * inner)]
    return lax.ppermute(x, ("lo", "tp"), list(zip(spot[:-by], spot[by:])))


def carried_in(contribution, log_span_decay):
    length = lax.axis_size(SPANS)
    state = from_behind(contribution.astype(jnp.bfloat16), 1).astype(jnp.float32)
    by = 1
    while by < length:
        earlier = from_behind(state.astype(jnp.bfloat16), by).astype(jnp.float32)
        state = state + jnp.exp(log_span_decay * by)[:, None, None] * earlier
        by *= 2
    return state


def spread_kernel(count, *refs):
    rows_ref, blocks = refs[0], refs[1 : 1 + count]
    tokens_out, fulls = refs[1 + count], refs[2 + count : 2 + 2 * count]
    passing = refs[2 + 2 * count : 2 + 3 * count]
    bounce = refs[2 + 3 * count : 2 + 4 * count]
    rows_bounce, send, arrive, arrive_pass, send_rows, arrive_rows, own = refs[2 + 4 * count :]
    hi, lo, tp = lax.axis_index("hi"), lax.axis_index("lo"), lax.axis_index("tp")
    planes = lax.axis_size("hi")
    side, core = tp // 2, tp % 2
    far_side = 1 - side
    across = (hi, lo, 2 * far_side + core)
    beside = (hi, 1 - lo, tp)
    sibling = (hi, lo, 2 * side + 1 - core)
    held = lax.rem(side + hi // 2, 2)
    other_held = 1 - held

    def remote(source, target, out_sem, in_sem, device):
        return pltpu.make_async_remote_copy(
            src_ref=source,
            dst_ref=target,
            send_sem=out_sem,
            recv_sem=in_sem,
            device_id=device,
            device_id_type=pl.DeviceIdType.MESH,
        )

    def via_vmem(source, buffer, target, done):
        inward = pltpu.make_async_copy(source, buffer, own)
        inward.start()
        inward.wait()
        pltpu.make_async_copy(buffer, target, done).start()

    def piece(k, source, row, half):
        depth = blocks[k].shape[0]
        start = (source * 2 + row) * depth + half * (depth // 2)
        return fulls[k].at[pl.ds(pl.multiple_of(start, depth // 2), depth // 2)]

    def half_of(k, half):
        depth = blocks[k].shape[0] // 2
        return blocks[k].at[pl.ds(half * depth, depth)]

    waits = []

    def push(k, source, row, half, slot, device):
        part = piece(k, source, row, half)
        copy = remote(part, part, send.at[k, slot], arrive.at[k, source, row, half], device)
        copy.start()
        waits.append(copy)

    def landed(k, source, row, half):
        part = piece(k, source, row, half)
        remote(part, part, send.at[k, 0], arrive.at[k, source, row, half], across).wait_recv()

    landing = pl.multiple_of(tp * rows_ref.shape[0], rows_ref.shape[0])
    my_rows = tokens_out.at[pl.ds(landing, rows_ref.shape[0])]

    for k in range(count):
        copy = remote(half_of(k, 1), passing[k], send.at[k, 0], arrive_pass.at[k], across)
        copy.start()
        waits.append(copy)

    def first_entry(k):
        return remote(
            half_of(k, 0),
            piece(k, hi, lo, 0),
            send.at[k, 1],
            arrive.at[k, hi, lo, 0],
            (tp, lo, 2 * side + lax.rem(hi, 2)),
        )

    def second_entry(k):
        return remote(
            passing[k],
            piece(k, hi, lo, 1),
            send.at[k, 2],
            arrive.at[k, hi, lo, 1],
            (2 * far_side + core, lo, 2 * side + lax.rem(hi, 2)),
        )

    def rows_copy(step):
        target = lax.rem(hi + step, planes)
        return remote(
            rows_ref, my_rows, send_rows.at[step], arrive_rows.at[tp], (target, lo, hi)
        )

    stays_first = tp == hi
    stays_second = 2 * far_side + core == hi
    for k in range(count):

        @pl.when(jnp.logical_not(stays_first))
        def _():
            first_entry(k).start()

    for step in range(1, 4):
        rows_copy(step).start()

    @pl.when(jnp.logical_not(stays_first))
    def _():
        rows_copy(0).start()

    @pl.when(stays_first)
    def _():
        via_vmem(rows_ref, rows_bounce, my_rows, arrive_rows.at[tp])
        for k in range(count):
            via_vmem(half_of(k, 0), bounce[k], piece(k, hi, lo, 0), arrive.at[k, hi, lo, 0])

    for k in range(count):
        remote(passing[k], passing[k], send.at[k, 0], arrive_pass.at[k], across).wait_recv()

        @pl.when(jnp.logical_not(stays_second))
        def _():
            second_entry(k).start()

        @pl.when(stays_second)
        def _():
            via_vmem(passing[k], bounce[k], piece(k, hi, lo, 1), arrive.at[k, hi, lo, 1])

    def own_step(k):
        for n in range(2):
            source = core + 2 * n
            landed(k, source, lo, held)
            push(k, source, lo, held, 3 + 3 * n, across)
            push(k, source, lo, held, 4 + 3 * n, beside)
            push(k, source, lo, held, 5 + 3 * n, sibling)

    def near_step(k):
        landed(k, core, lo, other_held)
        push(k, core, lo, other_held, 9, beside)
        push(k, core, lo, other_held, 10, sibling)
        landed(k, core + 2, 1 - lo, held)
        push(k, core + 2, 1 - lo, held, 11, across)
        push(k, core + 2, 1 - lo, held, 12, sibling)
        landed(k, core + 2, lo, other_held)
        push(k, core + 2, lo, other_held, 13, sibling)
        landed(k, core, 1 - lo, held)
        push(k, core, 1 - lo, held, 14, sibling)

    def far_step(k):
        landed(k, core, 1 - lo, other_held)
        push(k, core, 1 - lo, other_held, 15, sibling)
        landed(k, core + 2, 1 - lo, other_held)
        push(k, core + 2, 1 - lo, other_held, 16, sibling)

    for step in range(count + 2):
        if step < count:
            own_step(step)
        if 0 <= step - 1 < count:
            near_step(step - 1)
        if 0 <= step - 2:
            far_step(step - 2)

    for k in range(count):
        for n in range(2):
            for row in range(2):
                for half in range(2):
                    landed(k, 1 - core + 2 * n, row, half)
    for t in range(4):
        part = tokens_out.at[pl.ds(t * rows_ref.shape[0], rows_ref.shape[0])]
        remote(part, part, send_rows.at[0], arrive_rows.at[t], across).wait_recv()
    for copy in waits:
        copy.wait_send()
    for step in range(1, 4):
        rows_copy(step).wait_send()

    @pl.when(jnp.logical_not(stays_first))
    def _():
        rows_copy(0).wait_send()
        for k in range(count):
            first_entry(k).wait_send()

    @pl.when(jnp.logical_not(stays_second))
    def _():
        for k in range(count):
            second_entry(k).wait_send()


def spread(rows, blocks):
    count = len(blocks)
    shares = lax.axis_size(SPANS)
    halves = [(b.shape[0] // 2, b.shape[1]) for b in blocks]
    outs = [jax.ShapeDtypeStruct((4 * rows.shape[0], rows.shape[1]), rows.dtype)]
    outs += [jax.ShapeDtypeStruct((shares * b.shape[0], b.shape[1]), b.dtype) for b in blocks]
    outs += [jax.ShapeDtypeStruct(h, b.dtype) for h, b in zip(halves, blocks)]
    results = pl.pallas_call(
        lambda *refs: spread_kernel(count, *refs),
        out_shape=outs,
        in_specs=[pl.BlockSpec(memory_space=pl.ANY)] * (1 + count),
        out_specs=[pl.BlockSpec(memory_space=pl.ANY)] * len(outs),
        scratch_shapes=[pltpu.VMEM(h, b.dtype) for h, b in zip(halves, blocks)]
        + [
            pltpu.VMEM(rows.shape, rows.dtype),
            pltpu.SemaphoreType.DMA((count, 17)),
            pltpu.SemaphoreType.DMA((count, 4, 2, 2)),
            pltpu.SemaphoreType.DMA((count,)),
            pltpu.SemaphoreType.DMA((4,)),
            pltpu.SemaphoreType.DMA((4,)),
            pltpu.SemaphoreType.DMA,
        ],
        compiler_params=pltpu.CompilerParams(has_side_effects=True),
        name="spread",
    )(rows, *blocks)
    return results[0], results[1 : 1 + count]


def rms_normalize(tokens, norm_gain):
    widened = tokens.astype(jnp.float32)
    scaled = widened * lax.rsqrt(jnp.mean(widened * widened, axis=-1, keepdims=True) + rms_eps)
    return (scaled * norm_gain).astype(jnp.bfloat16)


def rotate(vectors, positions):
    half_width = vectors.shape[-1] // 2
    frequency = rope_base ** (-jnp.arange(half_width, dtype=jnp.float32) / half_width)
    angles = positions.astype(jnp.float32)[:, None] * frequency
    cosine = jnp.cos(angles)[:, None, :]
    sine_part = jnp.sin(angles)[:, None, :]
    front_half = vectors[..., :half_width]
    back_half = vectors[..., half_width:]
    return jnp.concatenate(
        [front_half * cosine - back_half * sine_part, front_half * sine_part + back_half * cosine],
        axis=-1,
    )


def prepare(queries, key_rows, values, positions):
    row_count = queries.shape[0]
    rotated_query = rotate(
        queries.astype(jnp.float32).reshape(row_count, -1, KEY), positions
    ).astype(jnp.bfloat16)
    rotated_keys = (
        rotate(key_rows.astype(jnp.float32).reshape(row_count, -1, KEY), positions) * KEY ** (-0.5)
    ).astype(jnp.bfloat16)
    value_heads = values.reshape(row_count, -1, VAL)
    return (rotated_query, rotated_keys, value_heads)


def decay_logs(first_head, head_total, all_heads, seq_length):
    ratio = (first_head + jnp.arange(head_total)).astype(jnp.float32) / (all_heads - 1)
    return (jnp.log(0.05) + ratio * jnp.log(18.0)) / seq_length


def local_parts(queries, key_rows, values, log_decay):
    row_count = queries.shape[0]
    indices = jnp.arange(row_count, dtype=jnp.float32)
    offsets = indices[:, None] - indices[None, :]
    causal = offsets >= 0
    weight = jnp.where(
        causal[None], jnp.exp(log_decay[:, None, None] * jnp.where(causal, offsets, 0.0)[None]), 0.0
    )
    scores = (
        jnp.einsum("ihd,jhd->hij", queries, key_rows, preferred_element_type=jnp.float32) * weight
    ).astype(jnp.bfloat16)
    within = jnp.einsum("hij,jhe->ihe", scores, values, preferred_element_type=jnp.float32)
    trailing = jnp.exp(log_decay[None, :] * (row_count - 1.0 - indices)[:, None])
    weighted = (key_rows.astype(jnp.float32) * trailing[:, :, None]).astype(jnp.bfloat16)
    contribution = jnp.einsum("jhd,jhe->hde", weighted, values, preferred_element_type=jnp.float32)
    return (within, contribution)


def cross_part(queries, carry_state, log_decay):
    row_count = queries.shape[0]
    indices = jnp.arange(row_count, dtype=jnp.float32)
    leading = jnp.exp(log_decay[None, :] * (indices + 1.0)[:, None])
    return (
        jnp.einsum(
            "ihd,hde->ihe",
            queries,
            carry_state.astype(jnp.bfloat16),
            preferred_element_type=jnp.float32,
        )
        * leading[:, :, None]
    )


def retain_finish(raw, switch):
    average = jnp.mean(raw, axis=-1, keepdims=True)
    spread = jnp.mean(jnp.square(raw - average), axis=-1, keepdims=True)
    normalized = ((raw - average) * lax.rsqrt(spread + group_eps)).reshape(raw.shape[0], -1)
    return (normalized * jax.nn.silu(switch.astype(jnp.float32))).astype(jnp.bfloat16)


def convolve_branch(gated_input, before, tap_slice, gain_slice, shift_slice, switch):
    padded = jnp.concatenate([before, gated_input], axis=0)
    row_count = gated_input.shape[0]
    summed = jnp.zeros(gated_input.shape, jnp.float32)
    for tap_index in range(tap_slice.shape[0]):
        summed = (
            summed
            + padded[tap_index : tap_index + row_count].astype(jnp.float32) * tap_slice[tap_index]
        )
    grouped = summed.reshape(row_count, -1, GROUP)
    average = jnp.mean(grouped, axis=-1, keepdims=True)
    spread = jnp.mean(jnp.square(grouped - average), axis=-1, keepdims=True)
    normalized = ((grouped - average) * lax.rsqrt(spread + layer_eps)).reshape(row_count, -1)
    normalized = normalized * gain_slice + shift_slice
    return (jax.nn.silu(normalized) * jax.nn.silu(switch.astype(jnp.float32))).astype(jnp.bfloat16)


def contract(hidden, matrix):
    return lax.dot_general(
        hidden, matrix, (((1,), (1,)), ((), ())), preferred_element_type=jnp.float32
    )


def local(
    tokens,
    norm_gain,
    query_weight,
    key_weight,
    value_weight,
    retain_gate,
    unit_value,
    unit_gate,
    convolve_gate,
    filter_taps,
    layer_gain,
    layer_shift,
    retain_output,
    convolve_output,
):
    head_groups = lax.axis_size("hi")
    chain_length = lax.axis_size(SPANS)
    head_rank = lax.axis_index("hi")
    chain_rank = lax.axis_index(SPANS)
    def project(rows, merged, *matrices):
        product = jnp.dot(rows, merged, preferred_element_type=jnp.float32).astype(jnp.bfloat16)
        ends = [sum(m.shape[1] for m in matrices[: k + 1]) for k in range(len(matrices) - 1)]
        return jnp.split(product, ends, axis=1)

    first = (key_weight, value_weight, query_weight)
    second = (unit_value, unit_gate, convolve_gate, retain_gate)
    third = (retain_output, convolve_output)
    groups = (first, second, third)
    merged = [jnp.concatenate(group, axis=1) for group in groups]
    normed = rms_normalize(tokens, norm_gain)
    if (lax.axis_size("lo"), lax.axis_size("tp")) == (2, 4):
        normed, merged = spread(normed, merged)
    else:
        normed = lax.all_gather(swap_planes(normed), "hi", axis=0, tiled=True)
        merged = [lax.all_gather(swap_planes(m), SPANS, axis=0, tiled=True) for m in merged]
    key_rows, values, queries = project(normed, merged[0], *first)
    glu_value, glu_switch, convolve_switch, retain_switch = project(normed, merged[1], *second)
    out_full = merged[2]
    row_count = normed.shape[0]
    local_heads = queries.shape[1] // KEY
    positions = chain_rank * row_count + jnp.arange(row_count, dtype=jnp.int32)
    rotated_query, rotated_keys, value_heads = prepare(queries, key_rows, values, positions)
    log_decay = decay_logs(
        head_rank * local_heads, local_heads, local_heads * head_groups, row_count * chain_length
    )
    within, contribution = local_parts(rotated_query, rotated_keys, value_heads, log_decay)
    gated_input = (
        glu_value.astype(jnp.float32) * jax.nn.sigmoid(glu_switch.astype(jnp.float32))
    ).astype(jnp.bfloat16)
    channels = gated_input.shape[1]
    before = from_behind(gated_input[row_count - (KW - 1) :], 1)
    incoming = carried_in(contribution, log_decay * row_count)
    raw = within + cross_part(rotated_query, incoming, log_decay)
    retain_hidden = retain_finish(raw, retain_switch)
    tap_slice = lax.dynamic_slice_in_dim(filter_taps, head_rank * channels, channels, 1)
    gain_slice = lax.dynamic_slice_in_dim(layer_gain, head_rank * channels, channels, 0)
    shift_slice = lax.dynamic_slice_in_dim(layer_shift, head_rank * channels, channels, 0)
    convolve_hidden = convolve_branch(
        gated_input, before, tap_slice, gain_slice, shift_slice, convolve_switch
    )
    hidden = jnp.concatenate([retain_hidden, convolve_hidden], axis=1)
    mixed = contract(hidden, out_full).astype(jnp.bfloat16)
    return swap_planes(lax.psum_scatter(mixed, "hi", scatter_dimension=0, tiled=True))


def solution(mesh):
    sp, tp = mesh.shape["sp"], mesh.shape["tp"]
    planes = Mesh(mesh.devices.reshape(tp, sp // tp, tp), ("hi", "lo", "tp"))
    return jax.shard_map(
        local,
        mesh=planes,
        in_specs=(
            P(("hi", "lo", "tp"), None),
            P(),
            P(("hi", "lo"), "tp"),
            P(("hi", "lo"), "tp"),
            P(("hi", "lo"), "tp"),
            P(("hi", "lo"), "tp"),
            P(("hi", "lo"), "tp"),
            P(("hi", "lo"), "tp"),
            P(("hi", "lo"), "tp"),
            P(),
            P(),
            P(),
            P(("hi", "lo"), "tp"),
            P(("hi", "lo"), "tp"),
        ),
        out_specs=P(("hi", "lo", "tp"), None),
        check_vma=False,
    )
```

```python
import jax
import jax.numpy as jnp
from jax import lax
from jax.experimental import pallas as pl
from jax.experimental.pallas import tpu as pltpu
from jax.sharding import Mesh
from jax.sharding import PartitionSpec as P

KEY = 256
VAL = 512
GROUP = 512
KW = 31


rms_eps = 1e-06
group_eps = 1.0
layer_eps = 0.001
rope_base = 10000.0


SPANS = ("tp", "lo")


def swap_planes(x):
    size = lax.axis_size("tp")
    pairs = [(h * size + t, t * size + h) for h in range(size) for t in range(size)]
    return lax.ppermute(x, ("hi", "tp"), pairs)


def from_behind(x, by):
    outer, inner = lax.axis_size("tp"), lax.axis_size("lo")
    spot = [(i % inner) * outer + i // inner for i in range(outer * inner)]
    return lax.ppermute(x, ("lo", "tp"), list(zip(spot[:-by], spot[by:])))


def carried_in(contribution, log_span_decay):
    length = lax.axis_size(SPANS)
    state = from_behind(contribution.astype(jnp.bfloat16), 1).astype(jnp.float32)
    by = 1
    while by < length:
        earlier = from_behind(state.astype(jnp.bfloat16), by).astype(jnp.float32)
        state = state + jnp.exp(log_span_decay * by)[:, None, None] * earlier
        by *= 2
    return state


def spread_kernel(count, *refs):
    rows_ref, blocks = refs[0], refs[1 : 1 + count]
    tokens_out, fulls = refs[1 + count], refs[2 + count : 2 + 2 * count]
    passing = refs[2 + 2 * count : 2 + 3 * count]
    bounce = refs[2 + 3 * count : 2 + 4 * count]
    rows_bounce, send, arrive, arrive_pass, send_rows, arrive_rows, own = refs[2 + 4 * count :]
    hi, lo, tp = lax.axis_index("hi"), lax.axis_index("lo"), lax.axis_index("tp")
    planes = lax.axis_size("hi")
    side, core = tp // 2, tp % 2
    far_side = 1 - side
    across = (hi, lo, 2 * far_side + core)
    beside = (hi, 1 - lo, tp)
    sibling = (hi, lo, 2 * side + 1 - core)
    held = lax.rem(side + hi // 2, 2)
    other_held = 1 - held

    def remote(source, target, out_sem, in_sem, device):
        return pltpu.make_async_remote_copy(
            src_ref=source,
            dst_ref=target,
            send_sem=out_sem,
            recv_sem=in_sem,
            device_id=device,
            device_id_type=pl.DeviceIdType.MESH,
        )

    def via_vmem(source, buffer, target, done):
        inward = pltpu.make_async_copy(source, buffer, own)
        inward.start()
        inward.wait()
        pltpu.make_async_copy(buffer, target, done).start()

    def piece(k, source, row, half):
        depth = blocks[k].shape[0]
        start = (source * 2 + row) * depth + half * (depth // 2)
        return fulls[k].at[pl.ds(pl.multiple_of(start, depth // 2), depth // 2)]

    def half_of(k, half):
        depth = blocks[k].shape[0] // 2
        return blocks[k].at[pl.ds(half * depth, depth)]

    waits = []

    def push(k, source, row, half, slot, device):
        part = piece(k, source, row, half)
        copy = remote(part, part, send.at[k, slot], arrive.at[k, source, row, half], device)
        copy.start()
        waits.append(copy)

    def landed(k, source, row, half):
        part = piece(k, source, row, half)
        remote(part, part, send.at[k, 0], arrive.at[k, source, row, half], across).wait_recv()

    landing = pl.multiple_of(tp * rows_ref.shape[0], rows_ref.shape[0])
    my_rows = tokens_out.at[pl.ds(landing, rows_ref.shape[0])]

    for k in range(count):
        copy = remote(half_of(k, 1), passing[k], send.at[k, 0], arrive_pass.at[k], across)
        copy.start()
        waits.append(copy)

    def first_entry(k):
        return remote(
            half_of(k, 0),
            piece(k, hi, lo, 0),
            send.at[k, 1],
            arrive.at[k, hi, lo, 0],
            (tp, lo, 2 * side + lax.rem(hi, 2)),
        )

    def second_entry(k):
        return remote(
            passing[k],
            piece(k, hi, lo, 1),
            send.at[k, 2],
            arrive.at[k, hi, lo, 1],
            (2 * far_side + core, lo, 2 * side + lax.rem(hi, 2)),
        )

    def rows_copy(step):
        target = lax.rem(hi + step, planes)
        return remote(
            rows_ref, my_rows, send_rows.at[step], arrive_rows.at[tp], (target, lo, hi)
        )

    stays_first = tp == hi
    stays_second = 2 * far_side + core == hi
    for k in range(count):

        @pl.when(jnp.logical_not(stays_first))
        def _():
            first_entry(k).start()

    for step in range(1, 4):
        rows_copy(step).start()

    @pl.when(jnp.logical_not(stays_first))
    def _():
        rows_copy(0).start()

    @pl.when(stays_first)
    def _():
        via_vmem(rows_ref, rows_bounce, my_rows, arrive_rows.at[tp])
        for k in range(count):
            via_vmem(half_of(k, 0), bounce[k], piece(k, hi, lo, 0), arrive.at[k, hi, lo, 0])

    for k in range(count):
        remote(passing[k], passing[k], send.at[k, 0], arrive_pass.at[k], across).wait_recv()

        @pl.when(jnp.logical_not(stays_second))
        def _():
            second_entry(k).start()

        @pl.when(stays_second)
        def _():
            via_vmem(passing[k], bounce[k], piece(k, hi, lo, 1), arrive.at[k, hi, lo, 1])

    def own_step(k):
        for n in range(2):
            source = core + 2 * n
            landed(k, source, lo, held)
            push(k, source, lo, held, 3 + 3 * n, across)
            push(k, source, lo, held, 4 + 3 * n, beside)
            push(k, source, lo, held, 5 + 3 * n, sibling)

    def near_step(k):
        landed(k, core, lo, other_held)
        push(k, core, lo, other_held, 9, beside)
        push(k, core, lo, other_held, 10, sibling)
        landed(k, core + 2, lo, other_held)
        if k < count - 1:
            push(k, core + 2, lo, other_held, 11, beside)
        push(k, core + 2, lo, other_held, 12, sibling)
        landed(k, core + 2, 1 - lo, held)
        if k == count - 1:
            push(k, core + 2, 1 - lo, held, 11, across)
        push(k, core + 2, 1 - lo, held, 13, sibling)
        landed(k, core, 1 - lo, held)
        push(k, core, 1 - lo, held, 14, sibling)

    def far_step(k):
        landed(k, core, 1 - lo, other_held)
        push(k, core, 1 - lo, other_held, 15, sibling)
        landed(k, core + 2, 1 - lo, other_held)
        push(k, core + 2, 1 - lo, other_held, 16, sibling)

    for step in range(count + 2):
        if step < count:
            own_step(step)
        if 0 <= step - 1 < count:
            near_step(step - 1)
        if 0 <= step - 2:
            far_step(step - 2)

    for k in range(count):
        for n in range(2):
            for row in range(2):
                for half in range(2):
                    landed(k, 1 - core + 2 * n, row, half)
    for t in range(4):
        part = tokens_out.at[pl.ds(t * rows_ref.shape[0], rows_ref.shape[0])]
        remote(part, part, send_rows.at[0], arrive_rows.at[t], across).wait_recv()
    for copy in waits:
        copy.wait_send()
    for step in range(1, 4):
        rows_copy(step).wait_send()

    @pl.when(jnp.logical_not(stays_first))
    def _():
        rows_copy(0).wait_send()
        for k in range(count):
            first_entry(k).wait_send()

    @pl.when(jnp.logical_not(stays_second))
    def _():
        for k in range(count):
            second_entry(k).wait_send()


def spread(rows, blocks):
    count = len(blocks)
    shares = lax.axis_size(SPANS)
    halves = [(b.shape[0] // 2, b.shape[1]) for b in blocks]
    outs = [jax.ShapeDtypeStruct((4 * rows.shape[0], rows.shape[1]), rows.dtype)]
    outs += [jax.ShapeDtypeStruct((shares * b.shape[0], b.shape[1]), b.dtype) for b in blocks]
    outs += [jax.ShapeDtypeStruct(h, b.dtype) for h, b in zip(halves, blocks)]
    results = pl.pallas_call(
        lambda *refs: spread_kernel(count, *refs),
        out_shape=outs,
        in_specs=[pl.BlockSpec(memory_space=pl.ANY)] * (1 + count),
        out_specs=[pl.BlockSpec(memory_space=pl.ANY)] * len(outs),
        scratch_shapes=[pltpu.VMEM(h, b.dtype) for h, b in zip(halves, blocks)]
        + [
            pltpu.VMEM(rows.shape, rows.dtype),
            pltpu.SemaphoreType.DMA((count, 17)),
            pltpu.SemaphoreType.DMA((count, 4, 2, 2)),
            pltpu.SemaphoreType.DMA((count,)),
            pltpu.SemaphoreType.DMA((4,)),
            pltpu.SemaphoreType.DMA((4,)),
            pltpu.SemaphoreType.DMA,
        ],
        compiler_params=pltpu.CompilerParams(has_side_effects=True),
        name="spread",
    )(rows, *blocks)
    return results[0], results[1 : 1 + count]


def rms_normalize(tokens, norm_gain):
    widened = tokens.astype(jnp.float32)
    scaled = widened * lax.rsqrt(jnp.mean(widened * widened, axis=-1, keepdims=True) + rms_eps)
    return (scaled * norm_gain).astype(jnp.bfloat16)


def rotate(vectors, positions):
    half_width = vectors.shape[-1] // 2
    frequency = rope_base ** (-jnp.arange(half_width, dtype=jnp.float32) / half_width)
    angles = positions.astype(jnp.float32)[:, None] * frequency
    cosine = jnp.cos(angles)[:, None, :]
    sine_part = jnp.sin(angles)[:, None, :]
    front_half = vectors[..., :half_width]
    back_half = vectors[..., half_width:]
    return jnp.concatenate(
        [front_half * cosine - back_half * sine_part, front_half * sine_part + back_half * cosine],
        axis=-1,
    )


def prepare(queries, key_rows, values, positions):
    row_count = queries.shape[0]
    rotated_query = rotate(
        queries.astype(jnp.float32).reshape(row_count, -1, KEY), positions
    ).astype(jnp.bfloat16)
    rotated_keys = (
        rotate(key_rows.astype(jnp.float32).reshape(row_count, -1, KEY), positions) * KEY ** (-0.5)
    ).astype(jnp.bfloat16)
    value_heads = values.reshape(row_count, -1, VAL)
    return (rotated_query, rotated_keys, value_heads)


def decay_logs(first_head, head_total, all_heads, seq_length):
    ratio = (first_head + jnp.arange(head_total)).astype(jnp.float32) / (all_heads - 1)
    return (jnp.log(0.05) + ratio * jnp.log(18.0)) / seq_length


def local_parts(queries, key_rows, values, log_decay):
    row_count = queries.shape[0]
    indices = jnp.arange(row_count, dtype=jnp.float32)
    offsets = indices[:, None] - indices[None, :]
    causal = offsets >= 0
    weight = jnp.where(
        causal[None], jnp.exp(log_decay[:, None, None] * jnp.where(causal, offsets, 0.0)[None]), 0.0
    )
    scores = (
        jnp.einsum("ihd,jhd->hij", queries, key_rows, preferred_element_type=jnp.float32) * weight
    ).astype(jnp.bfloat16)
    within = jnp.einsum("hij,jhe->ihe", scores, values, preferred_element_type=jnp.float32)
    trailing = jnp.exp(log_decay[None, :] * (row_count - 1.0 - indices)[:, None])
    weighted = (key_rows.astype(jnp.float32) * trailing[:, :, None]).astype(jnp.bfloat16)
    contribution = jnp.einsum("jhd,jhe->hde", weighted, values, preferred_element_type=jnp.float32)
    return (within, contribution)


def cross_part(queries, carry_state, log_decay):
    row_count = queries.shape[0]
    indices = jnp.arange(row_count, dtype=jnp.float32)
    leading = jnp.exp(log_decay[None, :] * (indices + 1.0)[:, None])
    return (
        jnp.einsum(
            "ihd,hde->ihe",
            queries,
            carry_state.astype(jnp.bfloat16),
            preferred_element_type=jnp.float32,
        )
        * leading[:, :, None]
    )


def retain_finish(raw, switch):
    average = jnp.mean(raw, axis=-1, keepdims=True)
    spread = jnp.mean(jnp.square(raw - average), axis=-1, keepdims=True)
    normalized = ((raw - average) * lax.rsqrt(spread + group_eps)).reshape(raw.shape[0], -1)
    return (normalized * jax.nn.silu(switch.astype(jnp.float32))).astype(jnp.bfloat16)


def convolve_branch(gated_input, before, tap_slice, gain_slice, shift_slice, switch):
    padded = jnp.concatenate([before, gated_input], axis=0)
    row_count = gated_input.shape[0]
    summed = jnp.zeros(gated_input.shape, jnp.float32)
    for tap_index in range(tap_slice.shape[0]):
        summed = (
            summed
            + padded[tap_index : tap_index + row_count].astype(jnp.float32) * tap_slice[tap_index]
        )
    grouped = summed.reshape(row_count, -1, GROUP)
    average = jnp.mean(grouped, axis=-1, keepdims=True)
    spread = jnp.mean(jnp.square(grouped - average), axis=-1, keepdims=True)
    normalized = ((grouped - average) * lax.rsqrt(spread + layer_eps)).reshape(row_count, -1)
    normalized = normalized * gain_slice + shift_slice
    return (jax.nn.silu(normalized) * jax.nn.silu(switch.astype(jnp.float32))).astype(jnp.bfloat16)


def contract(hidden, matrix):
    return lax.dot_general(
        hidden, matrix, (((1,), (1,)), ((), ())), preferred_element_type=jnp.float32
    )


def local(
    tokens,
    norm_gain,
    query_weight,
    key_weight,
    value_weight,
    retain_gate,
    unit_value,
    unit_gate,
    convolve_gate,
    filter_taps,
    layer_gain,
    layer_shift,
    retain_output,
    convolve_output,
):
    head_groups = lax.axis_size("hi")
    chain_length = lax.axis_size(SPANS)
    head_rank = lax.axis_index("hi")
    chain_rank = lax.axis_index(SPANS)
    def project(rows, merged, *matrices):
        product = jnp.dot(rows, merged, preferred_element_type=jnp.float32).astype(jnp.bfloat16)
        ends = [sum(m.shape[1] for m in matrices[: k + 1]) for k in range(len(matrices) - 1)]
        return jnp.split(product, ends, axis=1)

    groups = (
        (key_weight, query_weight),
        (value_weight,),
        (unit_value, unit_gate),
        (retain_gate,),
        (convolve_gate, convolve_output),
        (retain_output,),
    )
    merged = [jnp.concatenate(group, axis=1) for group in groups]
    normed = rms_normalize(tokens, norm_gain)
    if (lax.axis_size("lo"), lax.axis_size("tp")) == (2, 4):
        normed, merged = spread(normed, merged)
    else:
        normed = lax.all_gather(swap_planes(normed), "hi", axis=0, tiled=True)
        merged = [lax.all_gather(swap_planes(m), SPANS, axis=0, tiled=True) for m in merged]
    key_rows, queries = project(normed, merged[0], *groups[0])
    (values,) = project(normed, merged[1], *groups[1])
    glu_value, glu_switch = project(normed, merged[2], *groups[2])
    (retain_switch,) = project(normed, merged[3], *groups[3])
    gate_full, convolve_full = jnp.split(merged[4], [convolve_gate.shape[1]], axis=1)
    (convolve_switch,) = project(normed, gate_full, convolve_gate)
    retain_full = merged[5]
    row_count = normed.shape[0]
    local_heads = queries.shape[1] // KEY
    positions = chain_rank * row_count + jnp.arange(row_count, dtype=jnp.int32)
    rotated_query, rotated_keys, value_heads = prepare(queries, key_rows, values, positions)
    log_decay = decay_logs(
        head_rank * local_heads, local_heads, local_heads * head_groups, row_count * chain_length
    )
    within, contribution = local_parts(rotated_query, rotated_keys, value_heads, log_decay)
    gated_input = (
        glu_value.astype(jnp.float32) * jax.nn.sigmoid(glu_switch.astype(jnp.float32))
    ).astype(jnp.bfloat16)
    channels = gated_input.shape[1]
    before = from_behind(gated_input[row_count - (KW - 1) :], 1)
    incoming = carried_in(contribution, log_decay * row_count)
    raw = within + cross_part(rotated_query, incoming, log_decay)
    retain_hidden = retain_finish(raw, retain_switch)
    tap_slice = lax.dynamic_slice_in_dim(filter_taps, head_rank * channels, channels, 1)
    gain_slice = lax.dynamic_slice_in_dim(layer_gain, head_rank * channels, channels, 0)
    shift_slice = lax.dynamic_slice_in_dim(layer_shift, head_rank * channels, channels, 0)
    convolve_hidden = convolve_branch(
        gated_input, before, tap_slice, gain_slice, shift_slice, convolve_switch
    )
    mixed = (
        contract(retain_hidden, retain_full) + contract(convolve_hidden, convolve_full)
    ).astype(jnp.bfloat16)
    return swap_planes(lax.psum_scatter(mixed, "hi", scatter_dimension=0, tiled=True))


def solution(mesh):
    sp, tp = mesh.shape["sp"], mesh.shape["tp"]
    planes = Mesh(mesh.devices.reshape(tp, sp // tp, tp), ("hi", "lo", "tp"))
    return jax.shard_map(
        local,
        mesh=planes,
        in_specs=(
            P(("hi", "lo", "tp"), None),
            P(),
            P(("hi", "lo"), "tp"),
            P(("hi", "lo"), "tp"),
            P(("hi", "lo"), "tp"),
            P(("hi", "lo"), "tp"),
            P(("hi", "lo"), "tp"),
            P(("hi", "lo"), "tp"),
            P(("hi", "lo"), "tp"),
            P(),
            P(),
            P(),
            P(("hi", "lo"), "tp"),
            P(("hi", "lo"), "tp"),
        ),
        out_specs=P(("hi", "lo", "tp"), None),
        check_vma=False,
    )
```

```python
import jax
import jax.numpy as jnp
from jax import lax
from jax.experimental import pallas as pl
from jax.experimental.pallas import tpu as pltpu
from jax.sharding import Mesh
from jax.sharding import PartitionSpec as P

KEY = 256
VAL = 512
GROUP = 512
KW = 31


rms_eps = 1e-06
group_eps = 1.0
layer_eps = 0.001
rope_base = 10000.0


SPANS = ("tp", "lo")


def swap_planes(x):
    size = lax.axis_size("tp")
    pairs = [(h * size + t, t * size + h) for h in range(size) for t in range(size)]
    return lax.ppermute(x, ("hi", "tp"), pairs)


def from_behind(x, by):
    outer, inner = lax.axis_size("tp"), lax.axis_size("lo")
    spot = [(i % inner) * outer + i // inner for i in range(outer * inner)]
    return lax.ppermute(x, ("lo", "tp"), list(zip(spot[:-by], spot[by:])))


def carried_in(contribution, log_span_decay):
    length = lax.axis_size(SPANS)
    state = from_behind(contribution.astype(jnp.bfloat16), 1).astype(jnp.float32)
    by = 1
    while by < length:
        earlier = from_behind(state.astype(jnp.bfloat16), by).astype(jnp.float32)
        state = state + jnp.exp(log_span_decay * by)[:, None, None] * earlier
        by *= 2
    return state


def spread_kernel(count, *refs):
    rows_ref, blocks = refs[0], refs[1 : 1 + count]
    tokens_out, fulls = refs[1 + count], refs[2 + count : 2 + 2 * count]
    passing = refs[2 + 2 * count : 2 + 3 * count]
    bounce = refs[2 + 3 * count : 2 + 4 * count]
    rows_bounce, send, arrive, arrive_pass, send_rows, arrive_rows, own = refs[2 + 4 * count :]
    hi, lo, tp = lax.axis_index("hi"), lax.axis_index("lo"), lax.axis_index("tp")
    planes = lax.axis_size("hi")
    side, core = tp // 2, tp % 2
    far_side = 1 - side
    across = (hi, lo, 2 * far_side + core)
    beside = (hi, 1 - lo, tp)
    sibling = (hi, lo, 2 * side + 1 - core)
    held = lax.rem(side + hi // 2, 2)
    other_held = 1 - held

    def remote(source, target, out_sem, in_sem, device):
        return pltpu.make_async_remote_copy(
            src_ref=source,
            dst_ref=target,
            send_sem=out_sem,
            recv_sem=in_sem,
            device_id=device,
            device_id_type=pl.DeviceIdType.MESH,
        )

    def via_vmem(source, buffer, target, done):
        inward = pltpu.make_async_copy(source, buffer, own)
        inward.start()
        inward.wait()
        pltpu.make_async_copy(buffer, target, done).start()

    def piece(k, source, row, half):
        depth = blocks[k].shape[0]
        start = (source * 2 + row) * depth + half * (depth // 2)
        return fulls[k].at[pl.ds(pl.multiple_of(start, depth // 2), depth // 2)]

    def half_of(k, half):
        depth = blocks[k].shape[0] // 2
        return blocks[k].at[pl.ds(half * depth, depth)]

    waits = []

    def push(k, source, row, half, slot, device):
        part = piece(k, source, row, half)
        copy = remote(part, part, send.at[k, slot], arrive.at[k, source, row, half], device)
        copy.start()
        waits.append(copy)

    def landed(k, source, row, half):
        part = piece(k, source, row, half)
        remote(part, part, send.at[k, 0], arrive.at[k, source, row, half], across).wait_recv()

    landing = pl.multiple_of(tp * rows_ref.shape[0], rows_ref.shape[0])
    my_rows = tokens_out.at[pl.ds(landing, rows_ref.shape[0])]

    for k in range(count):
        copy = remote(half_of(k, 1), passing[k], send.at[k, 0], arrive_pass.at[k], across)
        copy.start()
        waits.append(copy)

    def first_entry(k):
        return remote(
            half_of(k, 0),
            piece(k, hi, lo, 0),
            send.at[k, 1],
            arrive.at[k, hi, lo, 0],
            (tp, lo, 2 * side + lax.rem(hi, 2)),
        )

    def second_entry(k):
        return remote(
            passing[k],
            piece(k, hi, lo, 1),
            send.at[k, 2],
            arrive.at[k, hi, lo, 1],
            (2 * far_side + core, lo, 2 * side + lax.rem(hi, 2)),
        )

    def rows_copy(step):
        target = lax.rem(hi + step, planes)
        return remote(
            rows_ref, my_rows, send_rows.at[step], arrive_rows.at[tp], (target, lo, hi)
        )

    stays_first = tp == hi
    stays_second = 2 * far_side + core == hi
    for k in range(count):

        @pl.when(jnp.logical_not(stays_first))
        def _():
            first_entry(k).start()

    for step in range(1, 4):
        rows_copy(step).start()

    @pl.when(jnp.logical_not(stays_first))
    def _():
        rows_copy(0).start()

    @pl.when(stays_first)
    def _():
        via_vmem(rows_ref, rows_bounce, my_rows, arrive_rows.at[tp])
        for k in range(count):
            via_vmem(half_of(k, 0), bounce[k], piece(k, hi, lo, 0), arrive.at[k, hi, lo, 0])

    for k in range(count):
        remote(passing[k], passing[k], send.at[k, 0], arrive_pass.at[k], across).wait_recv()

        @pl.when(jnp.logical_not(stays_second))
        def _():
            second_entry(k).start()

        @pl.when(stays_second)
        def _():
            via_vmem(passing[k], bounce[k], piece(k, hi, lo, 1), arrive.at[k, hi, lo, 1])

    def own_step(k):
        for n in range(2):
            source = core + 2 * n
            landed(k, source, lo, held)
            push(k, source, lo, held, 3 + 3 * n, across)
            push(k, source, lo, held, 4 + 3 * n, beside)
            push(k, source, lo, held, 5 + 3 * n, sibling)

    def near_step(k):
        landed(k, core, lo, other_held)
        push(k, core, lo, other_held, 9, beside)
        push(k, core, lo, other_held, 10, sibling)
        landed(k, core + 2, lo, other_held)
        if k < count - 1:
            push(k, core + 2, lo, other_held, 11, beside)
        push(k, core + 2, lo, other_held, 12, sibling)
        landed(k, core + 2, 1 - lo, held)
        if k == count - 1:
            push(k, core + 2, 1 - lo, held, 11, across)
        push(k, core + 2, 1 - lo, held, 13, sibling)
        landed(k, core, 1 - lo, held)
        push(k, core, 1 - lo, held, 14, sibling)

    def far_step(k):
        landed(k, core, 1 - lo, other_held)
        push(k, core, 1 - lo, other_held, 15, sibling)
        landed(k, core + 2, 1 - lo, other_held)
        push(k, core + 2, 1 - lo, other_held, 16, sibling)

    for step in range(count + 2):
        if step < count:
            own_step(step)
        if 0 <= step - 1 < count:
            near_step(step - 1)
        if 0 <= step - 2:
            far_step(step - 2)

    for k in range(count):
        for n in range(2):
            for row in range(2):
                for half in range(2):
                    landed(k, 1 - core + 2 * n, row, half)
    for t in range(4):
        part = tokens_out.at[pl.ds(t * rows_ref.shape[0], rows_ref.shape[0])]
        remote(part, part, send_rows.at[0], arrive_rows.at[t], across).wait_recv()
    for copy in waits:
        copy.wait_send()
    for step in range(1, 4):
        rows_copy(step).wait_send()

    @pl.when(jnp.logical_not(stays_first))
    def _():
        rows_copy(0).wait_send()
        for k in range(count):
            first_entry(k).wait_send()

    @pl.when(jnp.logical_not(stays_second))
    def _():
        for k in range(count):
            second_entry(k).wait_send()


def spread(rows, blocks):
    count = len(blocks)
    shares = lax.axis_size(SPANS)
    halves = [(b.shape[0] // 2, b.shape[1]) for b in blocks]
    outs = [jax.ShapeDtypeStruct((4 * rows.shape[0], rows.shape[1]), rows.dtype)]
    outs += [jax.ShapeDtypeStruct((shares * b.shape[0], b.shape[1]), b.dtype) for b in blocks]
    outs += [jax.ShapeDtypeStruct(h, b.dtype) for h, b in zip(halves, blocks)]
    results = pl.pallas_call(
        lambda *refs: spread_kernel(count, *refs),
        out_shape=outs,
        in_specs=[pl.BlockSpec(memory_space=pl.ANY)] * (1 + count),
        out_specs=[pl.BlockSpec(memory_space=pl.ANY)] * len(outs),
        scratch_shapes=[pltpu.VMEM(h, b.dtype) for h, b in zip(halves, blocks)]
        + [
            pltpu.VMEM(rows.shape, rows.dtype),
            pltpu.SemaphoreType.DMA((count, 17)),
            pltpu.SemaphoreType.DMA((count, 4, 2, 2)),
            pltpu.SemaphoreType.DMA((count,)),
            pltpu.SemaphoreType.DMA((4,)),
            pltpu.SemaphoreType.DMA((4,)),
            pltpu.SemaphoreType.DMA,
        ],
        compiler_params=pltpu.CompilerParams(has_side_effects=True),
        name="spread",
    )(rows, *blocks)
    return results[0], results[1 : 1 + count]


def rms_normalize(tokens, norm_gain):
    widened = tokens.astype(jnp.float32)
    scaled = widened * lax.rsqrt(jnp.mean(widened * widened, axis=-1, keepdims=True) + rms_eps)
    return (scaled * norm_gain).astype(jnp.bfloat16)


def rotate(vectors, positions):
    half_width = vectors.shape[-1] // 2
    frequency = rope_base ** (-jnp.arange(half_width, dtype=jnp.float32) / half_width)
    angles = positions.astype(jnp.float32)[:, None] * frequency
    cosine = jnp.cos(angles)[:, None, :]
    sine_part = jnp.sin(angles)[:, None, :]
    front_half = vectors[..., :half_width]
    back_half = vectors[..., half_width:]
    return jnp.concatenate(
        [front_half * cosine - back_half * sine_part, front_half * sine_part + back_half * cosine],
        axis=-1,
    )


def prepare(queries, key_rows, values, positions):
    row_count = queries.shape[0]
    rotated_query = rotate(
        queries.astype(jnp.float32).reshape(row_count, -1, KEY), positions
    ).astype(jnp.bfloat16)
    rotated_keys = (
        rotate(key_rows.astype(jnp.float32).reshape(row_count, -1, KEY), positions) * KEY ** (-0.5)
    ).astype(jnp.bfloat16)
    value_heads = values.reshape(row_count, -1, VAL)
    return (rotated_query, rotated_keys, value_heads)


def decay_logs(first_head, head_total, all_heads, seq_length):
    ratio = (first_head + jnp.arange(head_total)).astype(jnp.float32) / (all_heads - 1)
    return (jnp.log(0.05) + ratio * jnp.log(18.0)) / seq_length


def local_parts(queries, key_rows, values, log_decay):
    row_count = queries.shape[0]
    indices = jnp.arange(row_count, dtype=jnp.float32)
    offsets = indices[:, None] - indices[None, :]
    causal = offsets >= 0
    weight = jnp.where(
        causal[None], jnp.exp(log_decay[:, None, None] * jnp.where(causal, offsets, 0.0)[None]), 0.0
    )
    scores = (
        jnp.einsum("ihd,jhd->hij", queries, key_rows, preferred_element_type=jnp.float32) * weight
    ).astype(jnp.bfloat16)
    within = jnp.einsum("hij,jhe->ihe", scores, values, preferred_element_type=jnp.float32)
    trailing = jnp.exp(log_decay[None, :] * (row_count - 1.0 - indices)[:, None])
    weighted = (key_rows.astype(jnp.float32) * trailing[:, :, None]).astype(jnp.bfloat16)
    contribution = jnp.einsum("jhd,jhe->hde", weighted, values, preferred_element_type=jnp.float32)
    return (within, contribution)


def cross_part(queries, carry_state, log_decay):
    row_count = queries.shape[0]
    indices = jnp.arange(row_count, dtype=jnp.float32)
    leading = jnp.exp(log_decay[None, :] * (indices + 1.0)[:, None])
    return (
        jnp.einsum(
            "ihd,hde->ihe",
            queries,
            carry_state.astype(jnp.bfloat16),
            preferred_element_type=jnp.float32,
        )
        * leading[:, :, None]
    )


def retain_finish(raw, switch):
    average = jnp.mean(raw, axis=-1, keepdims=True)
    spread = jnp.mean(jnp.square(raw - average), axis=-1, keepdims=True)
    normalized = ((raw - average) * lax.rsqrt(spread + group_eps)).reshape(raw.shape[0], -1)
    return (normalized * jax.nn.silu(switch.astype(jnp.float32))).astype(jnp.bfloat16)


def convolve_branch(gated_input, before, tap_slice, gain_slice, shift_slice, switch):
    padded = jnp.concatenate([before, gated_input], axis=0)
    row_count = gated_input.shape[0]
    summed = jnp.zeros(gated_input.shape, jnp.float32)
    for tap_index in range(tap_slice.shape[0]):
        summed = (
            summed
            + padded[tap_index : tap_index + row_count].astype(jnp.float32) * tap_slice[tap_index]
        )
    grouped = summed.reshape(row_count, -1, GROUP)
    average = jnp.mean(grouped, axis=-1, keepdims=True)
    spread = jnp.mean(jnp.square(grouped - average), axis=-1, keepdims=True)
    normalized = ((grouped - average) * lax.rsqrt(spread + layer_eps)).reshape(row_count, -1)
    normalized = normalized * gain_slice + shift_slice
    return (jax.nn.silu(normalized) * jax.nn.silu(switch.astype(jnp.float32))).astype(jnp.bfloat16)


def contract(hidden, matrix):
    return lax.dot_general(
        hidden, matrix, (((1,), (1,)), ((), ())), preferred_element_type=jnp.float32
    )


def local(
    tokens,
    norm_gain,
    query_weight,
    key_weight,
    value_weight,
    retain_gate,
    unit_value,
    unit_gate,
    convolve_gate,
    filter_taps,
    layer_gain,
    layer_shift,
    retain_output,
    convolve_output,
):
    head_groups = lax.axis_size("hi")
    chain_length = lax.axis_size(SPANS)
    head_rank = lax.axis_index("hi")
    chain_rank = lax.axis_index(SPANS)
    def project(rows, merged, *matrices):
        product = jnp.dot(rows, merged, preferred_element_type=jnp.float32).astype(jnp.bfloat16)
        ends = [sum(m.shape[1] for m in matrices[: k + 1]) for k in range(len(matrices) - 1)]
        return jnp.split(product, ends, axis=1)

    first = (key_weight, value_weight, query_weight)
    second = (unit_value, unit_gate, convolve_gate, retain_gate)
    third = (retain_output, convolve_output)
    groups = (first, second, third)
    merged = [jnp.concatenate(group, axis=1) for group in groups]
    normed = rms_normalize(tokens, norm_gain)
    if (lax.axis_size("lo"), lax.axis_size("tp")) == (2, 4):
        normed, merged = spread(normed, merged)
    else:
        normed = lax.all_gather(swap_planes(normed), "hi", axis=0, tiled=True)
        merged = [lax.all_gather(swap_planes(m), SPANS, axis=0, tiled=True) for m in merged]
    key_rows, values, queries = project(normed, merged[0], *first)
    glu_value, glu_switch, convolve_switch, retain_switch = project(normed, merged[1], *second)
    out_full = merged[2]
    row_count = normed.shape[0]
    local_heads = queries.shape[1] // KEY
    positions = chain_rank * row_count + jnp.arange(row_count, dtype=jnp.int32)
    rotated_query, rotated_keys, value_heads = prepare(queries, key_rows, values, positions)
    log_decay = decay_logs(
        head_rank * local_heads, local_heads, local_heads * head_groups, row_count * chain_length
    )
    within, contribution = local_parts(rotated_query, rotated_keys, value_heads, log_decay)
    gated_input = (
        glu_value.astype(jnp.float32) * jax.nn.sigmoid(glu_switch.astype(jnp.float32))
    ).astype(jnp.bfloat16)
    channels = gated_input.shape[1]
    before = from_behind(gated_input[row_count - (KW - 1) :], 1)
    incoming = carried_in(contribution, log_decay * row_count)
    raw = within + cross_part(rotated_query, incoming, log_decay)
    retain_hidden = retain_finish(raw, retain_switch)
    tap_slice = lax.dynamic_slice_in_dim(filter_taps, head_rank * channels, channels, 1)
    gain_slice = lax.dynamic_slice_in_dim(layer_gain, head_rank * channels, channels, 0)
    shift_slice = lax.dynamic_slice_in_dim(layer_shift, head_rank * channels, channels, 0)
    convolve_hidden = convolve_branch(
        gated_input, before, tap_slice, gain_slice, shift_slice, convolve_switch
    )
    hidden = jnp.concatenate([retain_hidden, convolve_hidden], axis=1)
    mixed = contract(hidden, out_full).astype(jnp.bfloat16)
    return swap_planes(lax.psum_scatter(mixed, "hi", scatter_dimension=0, tiled=True))


def solution(mesh):
    sp, tp = mesh.shape["sp"], mesh.shape["tp"]
    planes = Mesh(mesh.devices.reshape(tp, sp // tp, tp), ("hi", "lo", "tp"))
    return jax.shard_map(
        local,
        mesh=planes,
        in_specs=(
            P(("hi", "lo", "tp"), None),
            P(),
            P(("hi", "lo"), "tp"),
            P(("hi", "lo"), "tp"),
            P(("hi", "lo"), "tp"),
            P(("hi", "lo"), "tp"),
            P(("hi", "lo"), "tp"),
            P(("hi", "lo"), "tp"),
            P(("hi", "lo"), "tp"),
            P(),
            P(),
            P(),
            P(("hi", "lo"), "tp"),
            P(("hi", "lo"), "tp"),
        ),
        out_specs=P(("hi", "lo", "tp"), None),
        check_vma=False,
    )
```
